32 devices in a mesh: sp: 4 (over z), fs: 4 (over y, x), tp: 2 (over core).
Axes of the slice: x: 2, y: 2, z: 4, core: 2. Of those that a mesh axis runs over, the one named last changes fastest.
Arguments:
- output_gate_logits: bfloat16 [4, 512, 2048], P('fs', 'sp', 'tp'), may hold values from -6 to 6
- head_input_rows: bfloat16 [4, 512, 2048], P('fs', 'sp', 'tp'), may hold values from -6 to 6
- group_state_writes: bfloat16 [4, 512, 512], P('fs', 'sp', 'tp'), may hold values from -6 to 6
- group_state_reads: bfloat16 [4, 512, 512], P('fs', 'sp', 'tp'), may hold values from -6 to 6
- step_logits: float32 [4, 512, 32], P('fs', 'sp', 'tp'), may hold values from -5 to 5
- head_step_offset: float32 [32], P('tp'), may hold values from -3.5 to 1
- head_decay_logrates: float32 [32], P('tp'), may hold values from -11 to 0
- decay_extra_spikes: float32 [512, 32], P('sp', 'tp'), may hold values from -2.1 to 0
- head_input_taps: bfloat16 [4, 2048], P(None, 'tp'), may hold values from -3 to 3
- state_input_taps: bfloat16 [4, 512], P(None, 'tp'), may hold values from -3 to 3
- readout_filter_taps: bfloat16 [4, 512], P(None, 'tp'), may hold values from -3 to 3
- grouped_norm_scale: float32 [2048], P('tp'), may hold values from 0.1 to 1.9
- convolution_outer_gate: bfloat16 [4, 512, 1024], P('fs', 'sp', 'tp'), may hold values from -6 to 6
- convolution_inner_gate: bfloat16 [4, 512, 1024], P('fs', 'sp', 'tp'), may hold values from -6 to 6
- convolution_value_rows: bfloat16 [4, 512, 1024], P('fs', 'sp', 'tp'), may hold values from -6 to 6
- gated_filter_taps: bfloat16 [3, 1024], P(None, 'tp'), may hold values from -3.5 to 3.5
- state_output_rows: bfloat16 [2048, 2048], P('tp', 'fs'), may hold values from -0.09375 to 0.09375
- convolution_output_rows: bfloat16 [1024, 2048], P('tp', 'fs'), may hold values from -0.125 to 0.125
Outputs:
- layer_out: bfloat16 [4, 512, 2048], P('tp', 'sp', 'fs')
The draws below stay inside these ranges and needn't reach their ends.
All inputs are finite; a program needn't handle non-finite values.
Results may differ from the reference program's by a relative error of at most 0.012.
Values may be sent and summed in bfloat16 or wider, within the bound.
A program may use at most 64 MiB of HBM per device.

```python
import jax
import jax.numpy as jnp
from jax import lax

D = 2048
HEADS = 32
HEAD_DIM = 64
GROUPS = 4
STATE = 128
CHANNELS = 1024
BLOCK = 128
SSD_TAPS = 4
CONV_TAPS = 3
TOK_DEV = 128
LENGTH = 512
SEQS = 4


def slow_heads(key):
    share = HEADS // 2
    order = jax.random.permutation(jax.random.fold_in(key, 11), HEADS)
    return order < share


def draw_head_decay_logrates(key, part):
    slow = slow_heads(key)
    spread = jax.random.uniform(jax.random.fold_in(key, 12), (HEADS,), jnp.float32)
    slow_rate = (0.2 + 0.6 * spread) / (0.07 * LENGTH)
    fast_rate = 0.01 * jnp.exp(spread * jnp.log(3.3))
    return jnp.log(jnp.where(slow, slow_rate, fast_rate)).astype(jnp.float32)


def draw_head_step_offset(key, part):
    slow = slow_heads(key)
    spread = jax.random.uniform(jax.random.fold_in(key, 13), (HEADS,), jnp.float32)
    return jnp.where(slow, spread - 3.5, spread).astype(jnp.float32)


def draw_step_logits(key, part):
    blocks = LENGTH // TOK_DEV
    quiet_span = max(1, blocks // 4)
    noise = jnp.clip(jax.random.normal(jax.random.fold_in(key, 22), (SEQS, LENGTH, HEADS), jnp.float32), -4.0, 4.0)
    offset = jax.random.uniform(jax.random.fold_in(key, 23), (SEQS, blocks, 1, HEADS), jnp.float32, -1.0, 1.0)
    lowered = jax.random.uniform(jax.random.fold_in(key, 24), (SEQS, blocks, 1, HEADS), jnp.float32, -5.0, -3.5)
    begin = jax.random.randint(jax.random.fold_in(key, 25), (SEQS, 1), 0, blocks - quiet_span + 1)
    places = jnp.arange(blocks, dtype=jnp.int32)[None, :]
    quiet = jnp.logical_and(places >= begin, places < begin + quiet_span)
    offset = jnp.where(quiet[:, :, None, None], lowered, offset)
    factor = jnp.where(quiet[:, :, None, None], 0.5, 1.0) * jnp.ones((SEQS, blocks, 1, HEADS), jnp.float32)
    offset = jnp.broadcast_to(offset, (SEQS, blocks, TOK_DEV, HEADS)).reshape(SEQS, LENGTH, HEADS)
    factor = jnp.broadcast_to(factor, (SEQS, blocks, TOK_DEV, HEADS)).reshape(SEQS, LENGTH, HEADS)
    return jnp.clip(noise * factor + offset, -5.0, 5.0).astype(jnp.float32)


def draw_decay_extra_spikes(key, part):
    spots = jax.random.randint(jax.random.fold_in(key, 31), (3,), 0, LENGTH)
    sizes = -jax.random.uniform(jax.random.fold_in(key, 32), (3, HEADS), jnp.float32, 0.22, 0.69)
    places = jnp.arange(LENGTH, dtype=jnp.int32)
    match = places[:, None] == spots[None, :]
    return jnp.sum(jnp.where(match[:, :, None], sizes[None], 0.0), axis=1).astype(jnp.float32)


def steps_of(rng, dims, cuts, smallest, top_value):
    factor_of = 1.0
    for axis_at, shards_of in cuts:
        draws = jax.random.uniform(jax.random.fold_in(jax.random.fold_in(rng, 6), axis_at), (shards_of,), jnp.float32, smallest / len(cuts), top_value / len(cuts))
        factor_of = factor_of * jnp.repeat(jnp.exp(draws), dims[axis_at] // shards_of).reshape((-1,) + (1,) * (len(dims) - 1 - axis_at))
    return factor_of


def scatter_about(stream_key, shape, deviation, most, cuts=(), kind=jnp.bfloat16):
    result = jax.random.normal(stream_key, shape, jnp.float32) * deviation
    if len(cuts) > 0:
        result = steps_of(stream_key, shape, cuts, -0.22, 0.18) * result
    return jnp.clip(result, min=-most, max=most).astype(kind)


def setup_inputs(seed: int = 0) -> dict:
    splits = jax.random.split(jax.random.key(seed), 19)
    output_gate_logits = scatter_about(splits[0], (SEQS, LENGTH, HEADS * HEAD_DIM), 1.0, 6.0, ((0, 4), (1, 4), (2, 2)))
    head_input_rows = scatter_about(splits[1], (SEQS, LENGTH, HEADS * HEAD_DIM), 1.0, 6.0, ((0, 4), (1, 4), (2, 2)))
    group_state_writes = scatter_about(splits[2], (SEQS, LENGTH, GROUPS * STATE), 1.0, 6.0, ((0, 4), (1, 4), (2, 2)))
    group_state_reads = scatter_about(splits[3], (SEQS, LENGTH, GROUPS * STATE), 1.0, 6.0, ((0, 4), (1, 4), (2, 2)))
    step_logits = draw_step_logits(jax.random.fold_in(splits[18], 71), 0)
    head_step_offset = draw_head_step_offset(jax.random.fold_in(splits[18], 71), 0)
    head_decay_logrates = draw_head_decay_logrates(jax.random.fold_in(splits[18], 71), 0)
    decay_extra_spikes = draw_decay_extra_spikes(jax.random.fold_in(splits[18], 71), 0)
    head_input_taps = scatter_about(splits[8], (SSD_TAPS, HEADS * HEAD_DIM), SSD_TAPS ** -0.5, 3.0, ((1, 2),))
    state_input_taps = scatter_about(splits[9], (SSD_TAPS, GROUPS * STATE), SSD_TAPS ** -0.5, 3.0, ((1, 2),))
    readout_filter_taps = scatter_about(splits[10], (SSD_TAPS, GROUPS * STATE), SSD_TAPS ** -0.5, 3.0, ((1, 2),))
    grouped_norm_scale = jnp.clip(1.0 + 0.18 * jax.random.normal(splits[11], (HEADS * HEAD_DIM,), jnp.float32), 0.1, 1.9)
    convolution_outer_gate = scatter_about(splits[12], (SEQS, LENGTH, CHANNELS), 1.0, 6.0, ((0, 4), (1, 4), (2, 2)))
    convolution_inner_gate = scatter_about(splits[13], (SEQS, LENGTH, CHANNELS), 1.0, 6.0, ((0, 4), (1, 4), (2, 2)))
    convolution_value_rows = scatter_about(splits[14], (SEQS, LENGTH, CHANNELS), 1.0, 6.0, ((0, 4), (1, 4), (2, 2)))
    gated_filter_taps = scatter_about(splits[15], (CONV_TAPS, CHANNELS), CONV_TAPS ** -0.5, 3.5, ((1, 2),))
    state_output_rows = scatter_about(splits[16], (HEADS * HEAD_DIM, D), (2 * HEADS * HEAD_DIM) ** -0.5, 0.09375, ((0, 2), (1, 4)))
    convolution_output_rows = scatter_about(splits[17], (CHANNELS, D), (2 * CHANNELS) ** -0.5, 0.125, ((0, 2), (1, 4)))
    return dict(output_gate_logits=output_gate_logits, head_input_rows=head_input_rows, group_state_writes=group_state_writes, group_state_reads=group_state_reads, step_logits=step_logits, head_step_offset=head_step_offset, head_decay_logrates=head_decay_logrates, decay_extra_spikes=decay_extra_spikes, head_input_taps=head_input_taps, state_input_taps=state_input_taps, readout_filter_taps=readout_filter_taps, grouped_norm_scale=grouped_norm_scale, convolution_outer_gate=convolution_outer_gate, convolution_inner_gate=convolution_inner_gate, convolution_value_rows=convolution_value_rows, gated_filter_taps=gated_filter_taps, state_output_rows=state_output_rows, convolution_output_rows=convolution_output_rows)


EPS = 1e-06
HIGH = lax.Precision.HIGHEST

def causal_filter(stream, kernel, before):
    span = kernel.shape[0]
    length = stream.shape[1]
    padded = jnp.concatenate([before, stream], axis=1)
    total = padded[:, 0:length] * kernel[0]
    for offset in range(1, span):
        total = total + padded[:, offset:offset + length] * kernel[offset]
    return total

def block_scan(driven, decay, writes, reads):
    batch, length, groups, ratio, channels = driven.shape
    entries = writes.shape[-1]
    count = length // BLOCK

    def split(array):
        shaped = array.reshape((batch, count, BLOCK) + array.shape[2:])
        return jnp.moveaxis(shaped, 1, 0)
    causal = jnp.tril(jnp.ones((BLOCK, BLOCK), dtype=bool))

    def advance(carry, pieces):
        drive, fall, write, read = pieces
        rising = jnp.cumsum(fall, axis=1)
        scores = jnp.einsum('blgn,bsgn->bgls', read, write, precision=HIGH)
        gaps = rising[:, :, None] - rising[:, None, :]
        weights = jnp.exp(jnp.where(causal[None, :, :, None, None], gaps, -jnp.inf))
        inside = jnp.einsum('bgls,blsgr,bsgrp->blgrp', scores, weights, drive, precision=HIGH)
        earlier = jnp.einsum('blgn,bgrpn->blgrp', read, carry, precision=HIGH) * jnp.exp(rising)[..., None]
        remain = jnp.exp(rising[:, -1:] - rising)
        fresh = jnp.einsum('bsgn,bsgr,bsgrp->bgrpn', write, remain, drive, precision=HIGH)
        carry = carry * jnp.exp(rising[:, -1])[..., None, None] + fresh
        return (carry, inside + earlier)
    start = jnp.zeros((batch, groups, ratio, channels, entries), jnp.float32)
    final, blocks = lax.scan(advance, start, (split(driven), split(decay), split(writes), split(reads)))
    return (final, jnp.moveaxis(blocks, 0, 1).reshape(driven.shape))

def reference(output_gate_logits, head_input_rows, group_state_writes, group_state_reads, step_logits, head_step_offset, head_decay_logrates, decay_extra_spikes, head_input_taps, state_input_taps, readout_filter_taps, grouped_norm_scale, convolution_outer_gate, convolution_inner_gate, convolution_value_rows, gated_filter_taps, state_output_rows, convolution_output_rows):
    ratio = HEADS // GROUPS

    def one_sequence(streams):
        gate, inputs, writes_raw, reads_raw, raw_step, outer, inner, values = streams
        length = inputs.shape[0]
        reach = head_input_taps.shape[0] - 1
        short = gated_filter_taps.shape[0] - 1
        filtered_input = jax.nn.silu(causal_filter(inputs[None].astype(jnp.float32), head_input_taps.astype(jnp.float32), jnp.zeros((1, reach, inputs.shape[1]), jnp.float32)))
        filtered_writes = jax.nn.silu(causal_filter(writes_raw[None].astype(jnp.float32), state_input_taps.astype(jnp.float32), jnp.zeros((1, reach, writes_raw.shape[1]), jnp.float32)))
        filtered_reads = jax.nn.silu(causal_filter(reads_raw[None].astype(jnp.float32), readout_filter_taps.astype(jnp.float32), jnp.zeros((1, reach, reads_raw.shape[1]), jnp.float32)))
        head_step_length = jax.nn.softplus(raw_step[None] + head_step_offset)
        decay_logarithm = decay_extra_spikes[None] - head_step_length * jnp.exp(head_decay_logrates)
        driven = (filtered_input.reshape(1, length, HEADS, HEAD_DIM) * head_step_length[..., None]).reshape(1, length, GROUPS, ratio, HEAD_DIM)
        final, state_output = block_scan(driven, decay_logarithm.reshape(1, length, GROUPS, ratio), filtered_writes.reshape(1, length, GROUPS, STATE), filtered_reads.reshape(1, length, GROUPS, STATE))
        gated = state_output.reshape(1, length, HEADS * HEAD_DIM) * jax.nn.silu(gate[None].astype(jnp.float32))
        grouped = gated.reshape(1, length, GROUPS, ratio * HEAD_DIM)
        normed = grouped * lax.rsqrt(lax.optimization_barrier(jnp.mean(grouped * grouped, axis=-1, keepdims=True)) + EPS)
        state_branch = (normed.reshape(1, length, HEADS * HEAD_DIM) * grouped_norm_scale).astype(jnp.bfloat16)
        product = inner[None].astype(jnp.float32) * values[None].astype(jnp.float32)
        filtered = causal_filter(product, gated_filter_taps.astype(jnp.float32), jnp.zeros((1, short, inner.shape[1]), jnp.float32))
        conv_branch = (outer[None].astype(jnp.float32) * filtered).astype(jnp.bfloat16)
        mixed = jnp.dot(state_branch[0], state_output_rows, preferred_element_type=jnp.float32) + jnp.dot(conv_branch[0], convolution_output_rows, preferred_element_type=jnp.float32)
        return mixed.astype(jnp.bfloat16)
    return lax.map(one_sequence, (output_gate_logits, head_input_rows, group_state_writes, group_state_reads, step_logits, convolution_outer_gate, convolution_inner_gate, convolution_value_rows))
```

```python
import functools

import jax
import jax.numpy as jnp
from jax import lax
from jax.experimental import pallas as pl
from jax.experimental.pallas import tpu as pltpu
from jax.sharding import PartitionSpec as P

STATE = 128
EPS = 1e-06
LANES = 128
HALO = 8
HIGH = lax.Precision.HIGHEST
MESH = pl.DeviceIdType.MESH
F32 = jnp.float32
BF16 = jnp.bfloat16


def mm(a, b):
    return jnp.dot(a, b, preferred_element_type=F32)


def silu(v):
    return v / (1.0 + jnp.exp(-v))


def kernel(
    sizes,
    gate_ref,
    head_ref,
    writes_ref,
    reads_ref,
    step_ref,
    offset_ref,
    rate_ref,
    spike_ref,
    head_taps,
    write_taps,
    read_taps,
    scale_ref,
    outer_ref,
    inner_ref,
    value_ref,
    conv_taps,
    wstate_hbm,
    wconv_hbm,
    out_ref,
    head_halo,
    write_halo,
    read_halo,
    inner_halo,
    value_halo,
    head_pad,
    group_pad,
    conv_pad,
    local_state,
    state_send,
    state_recv,
    inside,
    branch_send,
    branch_recv,
    conv_send,
    conv_recv,
    wstate,
    wconv,
    acc,
    halo_ss,
    halo_rs,
    state_ss,
    state_rs,
    branch_ss,
    branch_rs,
    conv_ss,
    conv_rs,
    weight_ss,
    weight_rs,
    local_sem,
):
    nsp, nfs, ntp = sizes
    sp, fs, tp = lax.axis_index("sp"), lax.axis_index("fs"), lax.axis_index("tp")
    length, width = head_ref.shape[1:]
    heads = step_ref.shape[2]
    channels = width // heads
    group_width = writes_ref.shape[2]
    groups = group_width // STATE
    ratio = heads // groups
    gw = ratio * channels
    per_tp = nfs // ntp
    chunks = width // LANES
    per_group = chunks // groups
    hpl = LANES // channels
    dest = fs // per_tp
    slot = lax.rem(fs, per_tp)
    first, last = sp == 0, sp == nsp - 1

    def at(s, f, t):
        return (s, f, t)

    barrier = pltpu.get_barrier_semaphore()
    for a in range(nfs):
        for b in range(ntp):
            if a == 0 and b == 0:
                continue
            pl.semaphore_signal(
                barrier,
                inc=1,
                device_id=at(sp, lax.rem(fs + a, nfs), lax.rem(tp + b, ntp)),
                device_id_type=MESH,
            )

    @pl.when(jnp.logical_not(first))
    def _():
        pl.semaphore_signal(barrier, inc=1, device_id=at(sp - 1, fs, tp), device_id_type=MESH)

    @pl.when(jnp.logical_not(last))
    def _():
        pl.semaphore_signal(barrier, inc=1, device_id=at(sp + 1, fs, tp), device_id_type=MESH)

    own_weights = [
        pltpu.make_async_copy(wstate_hbm, wstate.at[tp], local_sem.at[0]),
        pltpu.make_async_copy(wconv_hbm, wconv.at[tp], local_sem.at[1]),
    ]
    for copy in own_weights:
        copy.start()

    ends = jnp.minimum(sp, 1) + jnp.minimum(nsp - 1 - sp, 1)
    pl.semaphore_wait(barrier, nfs * ntp - 1 + ends)

    def remote(src, dst, ss, rs, device):
        return pltpu.make_async_remote_copy(
            src_ref=src, dst_ref=dst, send_sem=ss, recv_sem=rs, device_id=device, device_id_type=MESH
        )

    nxt = at(jnp.minimum(sp + 1, nsp - 1), fs, tp)
    tail = pl.ds(length - HALO, HALO)
    halos = [
        remote(src.at[0, tail, :], dst, halo_ss.at[k], halo_rs.at[k], nxt)
        for k, (src, dst) in enumerate(
            (
                (writes_ref, write_halo),
                (reads_ref, read_halo),
                (head_ref, head_halo),
                (inner_ref, inner_halo),
                (value_ref, value_halo),
            )
        )
    ]

    @pl.when(jnp.logical_not(last))
    def _():
        for copy in halos:
            copy.start()

    weights = []
    for b in range(1, ntp):
        other = at(sp, fs, lax.rem(tp + b, ntp))
        weights.append(
            remote(wconv_hbm, wconv.at[tp], weight_ss.at[b - 1, 0], weight_rs.at[b - 1, 0], other)
        )
        weights.append(
            remote(wstate_hbm, wstate.at[tp], weight_ss.at[b - 1, 1], weight_rs.at[b - 1, 1], other)
        )
    for copy in weights:
        copy.start()

    logits = step_ref[0] + offset_ref[...]
    dt = jnp.maximum(logits, 0.0) + jnp.log1p(jnp.exp(-jnp.abs(logits)))
    fall = spike_ref[...] - dt * jnp.exp(rate_ref[...])
    rows = lax.broadcasted_iota(jnp.int32, (length, length), 0)
    cols = lax.broadcasted_iota(jnp.int32, (length, length), 1)
    causal = cols <= rows
    rising = jnp.dot(
        causal.astype(F32), fall, precision=HIGH, preferred_element_type=F32
    )
    rising_t = rising.T
    dt_t = dt.T
    grow = jnp.exp(rising)
    left = dt * jnp.exp(rising[length - 1 : length] - rising)
    spread = (
        lax.broadcasted_iota(jnp.int32, (heads, width), 1) // channels
        == lax.broadcasted_iota(jnp.int32, (heads, width), 0)
    ).astype(BF16)
    stacked = jnp.concatenate([grow, left], axis=0)
    coarse = stacked.astype(BF16)
    fine = (stacked - coarse.astype(F32)).astype(BF16)
    wide = mm(coarse, spread) + mm(fine, spread)
    grow_wide, left_wide = wide[:length], wide[length:]
    last_wide = grow_wide[length - 1 : length]

    @pl.when(first)
    def _():
        for ref in (head_halo, write_halo, read_halo, inner_halo, value_halo):
            ref[...] = jnp.zeros_like(ref)

    @pl.when(jnp.logical_not(first))
    def _():
        for copy in halos:
            copy.wait_recv()

    def causal_filter(pad, stream, before, taps):
        span = taps.shape[0]
        pad[0:HALO, :] = before
        pad[HALO : HALO + length, :] = stream
        total = None
        for k in range(span):
            start = HALO - (span - 1) + k
            term = pad[start : start + length, :] * taps[k : k + 1]
            total = term if total is None else total + term
        return total

    writes = silu(
        causal_filter(
            group_pad, writes_ref[0].astype(F32), write_halo[...].astype(F32), write_taps[...].astype(F32)
        )
    )
    filtered = silu(
        causal_filter(
            head_pad, head_ref[0].astype(F32), head_halo[...].astype(F32), head_taps[...].astype(F32)
        )
    )
    writes_t = [
        writes[:, g * STATE : (g + 1) * STATE].T.astype(BF16) for g in range(groups)
    ]
    weighted = (filtered * left_wide).astype(BF16)
    for g in range(groups):
        piece = mm(writes_t[g], weighted[:, g * gw : (g + 1) * gw])
        for i in range(per_group):
            local_state[g * per_group + i] = piece[:, i * LANES : (i + 1) * LANES]

    chain = [
        remote(state_send.at[i], state_recv.at[i], state_ss.at[i], state_rs.at[i], nxt)
        for i in range(chunks)
    ]

    @pl.when(first)
    def _():
        for i in range(chunks):
            state_send[i] = local_state[i].astype(BF16)
        for copy in chain:
            copy.start()

    product = inner_ref[0].astype(F32) * value_ref[0].astype(F32)
    before = inner_halo[...].astype(F32) * value_halo[...].astype(F32)
    convolved = causal_filter(conv_pad, product, before, conv_taps[...].astype(F32))
    conv_rows = (outer_ref[0].astype(F32) * convolved).astype(BF16)
    conv_send[...] = conv_rows
    conv_copies = []
    for a in range(1, nfs):
        conv_copies.append(
            remote(
                conv_send,
                conv_recv.at[slot, tp],
                conv_ss.at[a],
                conv_rs.at[slot, tp],
                at(sp, lax.rem(fs + a, nfs), dest),
            )
        )
    for copy in conv_copies:
        copy.start()
    conv_home = remote(
        conv_send, conv_recv.at[slot, tp], conv_ss.at[0], conv_rs.at[slot, tp], at(sp, fs, dest)
    )

    @pl.when(dest == tp)
    def _():
        conv_recv[slot, tp] = conv_rows

    @pl.when(dest != tp)
    def _():
        conv_home.start()

    reads = silu(
        causal_filter(
            group_pad, reads_ref[0].astype(F32), read_halo[...].astype(F32), read_taps[...].astype(F32)
        )
    ).astype(BF16)
    filtered16 = filtered.astype(BF16)
    lane_head = lax.broadcasted_iota(jnp.int32, (length, LANES), 1) // channels
    for g in range(groups):
        scores = jnp.where(causal, mm(reads[:, g * STATE : (g + 1) * STATE], writes_t[g]), 0.0)
        for i in range(g * per_group, (g + 1) * per_group):
            block = filtered16[:, i * LANES : (i + 1) * LANES]
            total = None
            for r in range(hpl):
                h = i * hpl + r
                gaps = jnp.minimum(rising[:, h : h + 1] - rising_t[h : h + 1, :], 0.0)
                mixed = (scores * jnp.exp(gaps) * dt_t[h : h + 1, :]).astype(BF16)
                part = mm(mixed, block)
                total = part if total is None else jnp.where(lane_head == r, part, total)
            inside[:, i * LANES : (i + 1) * LANES] = total

    def branch_copy(g, a):
        return remote(
            branch_send.at[g],
            branch_recv.at[slot, tp, g],
            branch_ss.at[g, a],
            branch_rs.at[slot, tp, g],
            at(sp, lax.rem(fs + a, nfs), dest),
        )

    for g in range(groups):
        for i in range(g * per_group, (g + 1) * per_group):
            lanes = slice(i * LANES, (i + 1) * LANES)

            @pl.when(jnp.logical_not(first))
            def _():
                chain[i].wait_recv()
                incoming = state_recv[i]

                @pl.when(jnp.logical_not(last))
                def _():
                    state_send[i] = (
                        incoming.astype(F32) * last_wide[:, lanes] + local_state[i]
                    ).astype(BF16)
                    chain[i].start()

                inside[:, lanes] += (
                    mm(reads[:, g * STATE : (g + 1) * STATE], incoming) * grow_wide[:, lanes]
                )

        span = slice(g * gw, (g + 1) * gw)
        gated = inside[:, span] * silu(gate_ref[0, :, span].astype(F32))
        power = jnp.mean(gated * gated, axis=1, keepdims=True)
        normed = (gated * lax.rsqrt(power + EPS) * scale_ref[:, span]).astype(BF16)
        branch_send[g] = normed
        for a in range(1, nfs):
            branch_copy(g, a).start()

        @pl.when(dest == tp)
        def _():
            branch_recv[slot, tp, g] = normed

        @pl.when(dest != tp)
        def _():
            branch_copy(g, 0).start()

    for copy in own_weights:
        copy.wait()
    for copy in weights:
        copy.wait_recv()

    def local_source(j, c):
        return jnp.logical_and(fs == tp * per_tp + j, tp == c)

    for c in range(ntp):
        for j in range(per_tp):

            @pl.when(jnp.logical_not(local_source(j, c)))
            def _():
                remote(
                    conv_send, conv_recv.at[j, c], conv_ss.at[0], conv_rs.at[j, c], at(sp, fs, dest)
                ).wait_recv()

            term = mm(conv_recv[j, c], wconv[c])
            if c == 0:
                acc[j] = term
            else:
                acc[j] += term
    for g in range(groups):
        for c in range(ntp):
            for j in range(per_tp):

                @pl.when(jnp.logical_not(local_source(j, c)))
                def _():
                    remote(
                        branch_send.at[g],
                        branch_recv.at[j, c, g],
                        branch_ss.at[g, 0],
                        branch_rs.at[j, c, g],
                        at(sp, fs, dest),
                    ).wait_recv()

                acc[j] += mm(branch_recv[j, c, g], wstate[c, g * gw : (g + 1) * gw, :])
    for j in range(per_tp):
        out_ref[j] = acc[j].astype(BF16)

    @pl.when(jnp.logical_not(last))
    def _():
        for copy in halos:
            copy.wait_send()
        for copy in chain:
            copy.wait_send()

    for copy in weights:
        copy.wait_send()
    for copy in conv_copies:
        copy.wait_send()
    for g in range(groups):
        for a in range(1, nfs):
            branch_copy(g, a).wait_send()

    @pl.when(dest != tp)
    def _():
        conv_home.wait_send()
        for g in range(groups):
            branch_copy(g, 0).wait_send()


def per_device(sizes, *arrays):
    (
        gate,
        head,
        writes,
        reads,
        steps,
        offset,
        rates,
        spikes,
        head_taps,
        write_taps,
        read_taps,
        scale,
        outer,
        inner,
        value,
        conv_taps,
        wstate,
        wconv,
    ) = arrays
    nsp, nfs, ntp = sizes
    length, width = head.shape[1:]
    group_width = writes.shape[2]
    groups = group_width // STATE
    conv_width = inner.shape[2]
    features = wstate.shape[1]
    per_tp = nfs // ntp
    chunks = width // LANES
    vm = pl.BlockSpec(memory_space=pltpu.VMEM)
    hbm = pl.BlockSpec(memory_space=pl.ANY)
    dma = pltpu.SemaphoreType.DMA
    return pl.pallas_call(
        functools.partial(kernel, sizes),
        out_shape=jax.ShapeDtypeStruct((per_tp, length, features), BF16),
        in_specs=[vm] * 16 + [hbm] * 2,
        out_specs=vm,
        scratch_shapes=[
            pltpu.VMEM((HALO, width), BF16),
            pltpu.VMEM((HALO, group_width), BF16),
            pltpu.VMEM((HALO, group_width), BF16),
            pltpu.VMEM((HALO, conv_width), BF16),
            pltpu.VMEM((HALO, conv_width), BF16),
            pltpu.VMEM((HALO + length, width), F32),
            pltpu.VMEM((HALO + length, group_width), F32),
            pltpu.VMEM((HALO + length, conv_width), F32),
            pltpu.VMEM((chunks, STATE, LANES), F32),
            pltpu.VMEM((chunks, STATE, LANES), BF16),
            pltpu.VMEM((chunks, STATE, LANES), BF16),
            pltpu.VMEM((length, width), F32),
            pltpu.VMEM((groups, length, width // groups), BF16),
            pltpu.VMEM((per_tp, ntp, groups, length, width // groups), BF16),
            pltpu.VMEM((length, conv_width), BF16),
            pltpu.VMEM((per_tp, ntp, length, conv_width), BF16),
            pltpu.VMEM((ntp, width, features), BF16),
            pltpu.VMEM((ntp, conv_width, features), BF16),
            pltpu.VMEM((per_tp, length, features), F32),
            dma((5,)),
            dma((5,)),
            dma((chunks,)),
            dma((chunks,)),
            dma((groups, nfs)),
            dma((per_tp, ntp, groups)),
            dma((nfs,)),
            dma((per_tp, ntp)),
            dma((ntp - 1, 2)),
            dma((ntp - 1, 2)),
            dma((2,)),
        ],
        compiler_params=pltpu.CompilerParams(collective_id=0, has_side_effects=True),
    )(
        gate,
        head,
        writes,
        reads,
        steps,
        offset[None],
        rates[None],
        spikes,
        head_taps,
        write_taps,
        read_taps,
        scale[None],
        outer,
        inner,
        value,
        conv_taps,
        wstate,
        wconv,
    )


def solution(mesh):
    sizes = tuple(mesh.shape[name] for name in ("sp", "fs", "tp"))
    return jax.shard_map(
        functools.partial(per_device, sizes),
        mesh=mesh,
        in_specs=(
            P("fs", "sp", "tp"),
            P("fs", "sp", "tp"),
            P("fs", "sp", "tp"),
            P("fs", "sp", "tp"),
            P("fs", "sp", "tp"),
            P("tp"),
            P("tp"),
            P("sp", "tp"),
            P(None, "tp"),
            P(None, "tp"),
            P(None, "tp"),
            P("tp"),
            P("fs", "sp", "tp"),
            P("fs", "sp", "tp"),
            P("fs", "sp", "tp"),
            P(None, "tp"),
            P("tp", "fs"),
            P("tp", "fs"),
        ),
        out_specs=P("tp", "sp", "fs"),
        check_vma=False,
    )
```

```python
import functools

import jax
import jax.numpy as jnp
from jax import lax
from jax.experimental import pallas as pl
from jax.experimental.pallas import tpu as pltpu
from jax.sharding import PartitionSpec as P

STATE = 128
EPS = 1e-06
LANES = 128
HALO = 8
HIGH = lax.Precision.HIGHEST
MESH = pl.DeviceIdType.MESH
F32 = jnp.float32
BF16 = jnp.bfloat16


def mm(a, b):
    return jnp.dot(a, b, preferred_element_type=F32)


def silu(v):
    return v / (1.0 + jnp.exp(-v))


def kernel(
    sizes,
    gate_hbm,
    head_hbm,
    writes_hbm,
    reads_hbm,
    step_ref,
    offset_ref,
    rate_ref,
    spike_ref,
    head_taps,
    write_taps,
    read_taps,
    scale_ref,
    outer_hbm,
    inner_hbm,
    value_hbm,
    conv_taps,
    wstate_hbm,
    wconv_hbm,
    out_ref,
    gate_ref,
    head_ref,
    writes_ref,
    reads_ref,
    outer_ref,
    inner_ref,
    value_ref,
    head_halo,
    write_halo,
    read_halo,
    inner_halo,
    value_halo,
    head_pad,
    group_pad,
    conv_pad,
    local_state,
    state_send,
    state_recv,
    branch_send,
    branch_recv,
    norm_send,
    norm_recv,
    conv_send,
    conv_recv,
    wstate,
    wconv,
    acc,
    part,
    inside,
    input_sem,
    halo_ss,
    halo_rs,
    state_ss,
    state_rs,
    branch_ss,
    branch_rs,
    half_ss,
    half_rs,
    norm_ss,
    norm_rs,
    conv_ss,
    conv_rs,
    weight_ss,
    weight_rs,
    local_sem,
):
    nsp, nfs, ntp = sizes
    sp, fs, tp = lax.axis_index("sp"), lax.axis_index("fs"), lax.axis_index("tp")
    length, width = head_ref.shape[1:]
    heads = step_ref.shape[1]
    channels = width // heads
    group_width = writes_ref.shape[2]
    groups = group_width // STATE
    ratio = heads // groups
    gw = ratio * channels
    per_tp = nfs // ntp
    chunks = width // LANES
    per_group = chunks // groups
    hpl = LANES // channels
    per_unit = min(2, per_group)
    units = chunks // per_unit
    unit_width = per_unit * LANES
    half = length // 2
    dest = fs // per_tp
    slot = lax.rem(fs, per_tp)
    first, last = sp == 0, sp == nsp - 1

    def at(s, f, t):
        return (s, f, t)

    barrier = pltpu.get_barrier_semaphore()
    for a in range(nfs):
        for b in range(ntp):
            if a == 0 and b == 0:
                continue
            pl.semaphore_signal(
                barrier,
                inc=1,
                device_id=at(sp, lax.rem(fs + a, nfs), lax.rem(tp + b, ntp)),
                device_id_type=MESH,
            )

    @pl.when(jnp.logical_not(first))
    def _():
        pl.semaphore_signal(barrier, inc=1, device_id=at(sp - 1, fs, tp), device_id_type=MESH)

    @pl.when(jnp.logical_not(last))
    def _():
        pl.semaphore_signal(barrier, inc=1, device_id=at(sp + 1, fs, tp), device_id_type=MESH)

    inputs = [
        pltpu.make_async_copy(src, dst, input_sem.at[k])
        for k, (src, dst) in enumerate(
            (
                (writes_hbm, writes_ref),
                (reads_hbm, reads_ref),
                (head_hbm, head_ref),
                (inner_hbm, inner_ref),
                (value_hbm, value_ref),
                (outer_hbm, outer_ref),
                (gate_hbm, gate_ref),
            )
        )
    ]
    for copy in inputs:
        copy.start()

    own_weights = [
        pltpu.make_async_copy(wstate_hbm, wstate.at[tp], local_sem.at[0]),
        pltpu.make_async_copy(wconv_hbm, wconv.at[tp], local_sem.at[1]),
    ]
    for copy in own_weights:
        copy.start()

    ends = jnp.minimum(sp, 1) + jnp.minimum(nsp - 1 - sp, 1)
    for copy in inputs:
        copy.wait()
    pl.semaphore_wait(barrier, nfs * ntp - 1 + ends)

    def remote(src, dst, ss, rs, device):
        return pltpu.make_async_remote_copy(
            src_ref=src, dst_ref=dst, send_sem=ss, recv_sem=rs, device_id=device, device_id_type=MESH
        )

    nxt = at(jnp.minimum(sp + 1, nsp - 1), fs, tp)
    tail = pl.ds(length - HALO, HALO)
    halos = [
        remote(src.at[0, tail, :], dst, halo_ss.at[k], halo_rs.at[k], nxt)
        for k, (src, dst) in enumerate(
            (
                (writes_ref, write_halo),
                (reads_ref, read_halo),
                (head_ref, head_halo),
                (inner_ref, inner_halo),
                (value_ref, value_halo),
            )
        )
    ]

    @pl.when(jnp.logical_not(last))
    def _():
        for copy in halos:
            copy.start()

    weights = []
    for b in range(1, ntp):
        other = at(sp, fs, lax.rem(tp + b, ntp))
        weights.append(
            remote(wconv_hbm, wconv.at[tp], weight_ss.at[b - 1, 0], weight_rs.at[b - 1, 0], other)
        )
        weights.append(
            remote(wstate_hbm, wstate.at[tp], weight_ss.at[b - 1, 1], weight_rs.at[b - 1, 1], other)
        )
    for copy in weights:
        copy.start()

    def column(ref):
        return jnp.broadcast_to(ref[...], (length, heads)).T

    logits = step_ref[0] + column(offset_ref)
    dt_t = jnp.maximum(logits, 0.0) + jnp.log1p(jnp.exp(-jnp.abs(logits)))
    fall = spike_ref[...] - dt_t * jnp.exp(column(rate_ref))
    rows = lax.broadcasted_iota(jnp.int32, (length, length), 0)
    cols = lax.broadcasted_iota(jnp.int32, (length, length), 1)
    causal = cols <= rows
    rising_t = jnp.dot(
        fall, (rows <= cols).astype(F32), precision=HIGH, preferred_element_type=F32
    )
    rising = rising_t.T
    grow = jnp.exp(rising_t)
    left = dt_t * jnp.exp(rising_t[:, length - 1 : length] - rising_t)
    stacked = jnp.concatenate([grow, left], axis=0)
    coarse = stacked.astype(BF16).astype(F32)
    split = jnp.concatenate([coarse, stacked - coarse], axis=0).T.astype(BF16)
    spread = (
        lax.broadcasted_iota(jnp.int32, (4 * heads, 2 * width), 1) // channels
        == lax.broadcasted_iota(jnp.int32, (4 * heads, 2 * width), 0) % (2 * heads)
    ).astype(BF16)
    wide = mm(split, spread)
    grow_wide, left_wide = wide[:, :width], wide[:, width:]
    last_wide = grow_wide[length - 1 : length]

    @pl.when(first)
    def _():
        for ref in (head_halo, write_halo, read_halo, inner_halo, value_halo):
            ref[...] = jnp.zeros_like(ref)

    @pl.when(jnp.logical_not(first))
    def _():
        for copy in halos:
            copy.wait_recv()

    def causal_filter(pad, stream, before, taps):
        span = taps.shape[0]
        pad[0:HALO, :] = before
        pad[HALO : HALO + length, :] = stream
        total = None
        for k in range(span):
            start = HALO - (span - 1) + k
            term = pad[start : start + length, :] * taps[k : k + 1]
            total = term if total is None else total + term
        return total

    writes = silu(
        causal_filter(
            group_pad, writes_ref[0].astype(F32), write_halo[...].astype(F32), write_taps[...].astype(F32)
        )
    )
    filtered = silu(
        causal_filter(
            head_pad, head_ref[0].astype(F32), head_halo[...].astype(F32), head_taps[...].astype(F32)
        )
    )
    writes_t = [
        writes[:, g * STATE : (g + 1) * STATE].T.astype(BF16) for g in range(groups)
    ]
    weighted = (filtered * left_wide).astype(BF16)
    for g in range(groups):
        piece = mm(writes_t[g], weighted[:, g * gw : (g + 1) * gw])
        for i in range(per_group):
            local_state[g * per_group + i] = piece[:, i * LANES : (i + 1) * LANES]

    chain = [
        remote(state_send.at[i], state_recv.at[i], state_ss.at[i], state_rs.at[i], nxt)
        for i in range(chunks)
    ]

    @pl.when(first)
    def _():
        for i in range(chunks):
            state_send[i] = local_state[i].astype(BF16)
        for copy in chain:
            copy.start()

    product = inner_ref[0].astype(F32) * value_ref[0].astype(F32)
    before = inner_halo[...].astype(F32) * value_halo[...].astype(F32)
    convolved = causal_filter(conv_pad, product, before, conv_taps[...].astype(F32))
    conv_rows = (outer_ref[0].astype(F32) * convolved).astype(BF16)
    conv_send[...] = conv_rows
    conv_copies = []
    for a in range(1, nfs):
        conv_copies.append(
            remote(
                conv_send,
                conv_recv.at[slot, tp],
                conv_ss.at[a],
                conv_rs.at[slot, tp],
                at(sp, lax.rem(fs + a, nfs), dest),
            )
        )
    for copy in conv_copies:
        copy.start()
    conv_home = remote(
        conv_send, conv_recv.at[slot, tp], conv_ss.at[0], conv_rs.at[slot, tp], at(sp, fs, dest)
    )

    @pl.when(dest == tp)
    def _():
        conv_recv[slot, tp] = conv_rows

    @pl.when(dest != tp)
    def _():
        conv_home.start()

    reads = silu(
        causal_filter(
            group_pad, reads_ref[0].astype(F32), read_halo[...].astype(F32), read_taps[...].astype(F32)
        )
    ).astype(BF16)
    filtered16 = filtered.astype(BF16)
    lane_head = lax.broadcasted_iota(jnp.int32, (length, LANES), 1) // channels
    for g in range(groups):
        scores = jnp.where(causal, mm(reads[:, g * STATE : (g + 1) * STATE], writes_t[g]), 0.0)
        for i in range(g * per_group, (g + 1) * per_group):
            block = filtered16[:, i * LANES : (i + 1) * LANES]
            total = None
            for r in range(hpl):
                h = i * hpl + r
                gaps = jnp.minimum(rising[:, h : h + 1] - rising_t[h : h + 1, :], 0.0)
                mixed = (scores * jnp.exp(gaps) * dt_t[h : h + 1, :]).astype(BF16)
                one = mm(mixed, block)
                total = one if total is None else jnp.where(lane_head == r, one, total)
            inside[:, i * LANES : (i + 1) * LANES] = total

    home = dest == tp
    xfs = fs + 1 - 2 * lax.rem(fs, 2)
    yfs = lax.rem(fs + 2, nfs)
    pfs = nfs - 1 - fs

    def branch_copy(u, k, f):
        return remote(
            branch_send.at[u],
            branch_recv.at[slot, tp, u],
            branch_ss.at[u, k],
            branch_rs.at[slot, tp, u],
            at(sp, f, dest),
        )

    def norm_copy(g, k, f):
        return remote(
            norm_send.at[g],
            norm_recv.at[slot, tp, g],
            norm_ss.at[g, k],
            norm_rs.at[slot, tp, g],
            at(sp, f, dest),
        )

    for g in range(groups):
        span = slice(g * gw, (g + 1) * gw)
        power = jnp.zeros((length, LANES), F32)
        for i in range(g * per_group, (g + 1) * per_group):
            lanes = slice(i * LANES, (i + 1) * LANES)

            @pl.when(jnp.logical_not(first))
            def _():
                chain[i].wait_recv()
                incoming = state_recv[i]

                @pl.when(jnp.logical_not(last))
                def _():
                    state_send[i] = (
                        incoming.astype(F32) * last_wide[:, lanes] + local_state[i]
                    ).astype(BF16)
                    chain[i].start()

                inside[:, lanes] += (
                    mm(reads[:, g * STATE : (g + 1) * STATE], incoming) * grow_wide[:, lanes]
                )

            gated = inside[:, lanes] * silu(gate_ref[0, :, lanes].astype(F32))
            power = power + gated * gated
            u, at_lane = i // per_unit, (i % per_unit) * LANES
            scaled = (gated * scale_ref[:, lanes]).astype(BF16)
            branch_send[u, 0, :, at_lane : at_lane + LANES] = scaled[:half]
            branch_send[u, 1, :, at_lane : at_lane + LANES] = scaled[half:]
            if i % per_unit == per_unit - 1:
                branch_copy(u, 1, xfs).start()
                branch_copy(u, 2, yfs).start()

                @pl.when(home)
                def _():
                    branch_recv[slot, tp, u] = branch_send[u]

                @pl.when(jnp.logical_not(home))
                def _():
                    branch_copy(u, 0, fs).start()

        factor = lax.rsqrt(jnp.sum(power, axis=1, keepdims=True) / gw + EPS)
        factor = jnp.broadcast_to(factor, (length, LANES)).T[:8]
        norm_send[g] = factor
        norm_copy(g, 1, xfs).start()
        norm_copy(g, 2, yfs).start()
        norm_copy(g, 3, pfs).start()

        @pl.when(home)
        def _():
            norm_recv[slot, tp, g] = factor

        @pl.when(jnp.logical_not(home))
        def _():
            norm_copy(g, 0, fs).start()

    for copy in own_weights:
        copy.wait()
    for copy in weights:
        copy.wait_recv()

    def local_source(j, c):
        return jnp.logical_and(fs == tp * per_tp + j, tp == c)

    for c in range(ntp):
        for j in range(per_tp):

            @pl.when(jnp.logical_not(local_source(j, c)))
            def _():
                remote(
                    conv_send, conv_recv.at[j, c], conv_ss.at[0], conv_rs.at[j, c], at(sp, fs, dest)
                ).wait_recv()

            term = mm(conv_recv[j, c], wconv[c])
            if c == 0:
                acc[j] = term
            else:
                acc[j] += term
    own = lax.rem(fs, 2)
    side = jnp.where(home, 1 - own, own)
    upper = jnp.where(home, 0, 1)
    onward = at(sp, jnp.where(home, yfs, xfs), tp)

    def forward(c, u):
        return remote(
            branch_recv.at[side, c, u, upper],
            branch_recv.at[side, c, u, upper],
            half_ss.at[c, u],
            half_rs.at[upper, c, u],
            onward,
        )

    def arrived(j, c, u):
        remote(
            branch_send.at[u],
            branch_recv.at[j, c, u],
            branch_ss.at[u, 0],
            branch_rs.at[j, c, u],
            at(sp, xfs, dest),
        ).wait_recv()

    for u in range(units):
        for c in range(ntp):
            arrived(side, c, u)
            forward(c, u).start()

    def project(j, u, c):
        rows = branch_recv[j, c, u].reshape(length, unit_width)
        term = mm(rows, wstate[c, u * unit_width : (u + 1) * unit_width, :])
        if (u * per_unit) % per_group == 0:
            part[c] = term
        else:
            part[c] += term

    def finish(j, g, c):
        @pl.when(jnp.logical_not(local_source(j, c)))
        def _():
            remote(
                norm_send.at[g],
                norm_recv.at[j, c, g],
                norm_ss.at[g, 0],
                norm_rs.at[j, c, g],
                at(sp, xfs, dest),
            ).wait_recv()

        turned = jnp.broadcast_to(norm_recv[j, c, g][:1], (LANES, length)).T
        acc[j] += part[c] * turned[:, :1]

    per_norm = per_group // per_unit
    for j, straight in ((side, True), (1 - side, False)):
        for g in range(groups):
            for u in range(g * per_norm, (g + 1) * per_norm):
                for c in range(ntp):
                    if not straight:

                        @pl.when(jnp.logical_and(home, tp != c))
                        def _():
                            arrived(j, c, u)

                        @pl.when(jnp.logical_not(home))
                        def _():
                            for h in range(2):
                                remote(
                                    branch_send.at[u, h],
                                    branch_recv.at[j, c, u, h],
                                    half_ss.at[c, u],
                                    half_rs.at[h, c, u],
                                    onward,
                                ).wait_recv()

                    project(j, u, c)
            for c in range(ntp):
                finish(j, g, c)
    for j in range(per_tp):
        out_ref[j] = acc[j].astype(BF16)

    @pl.when(jnp.logical_not(last))
    def _():
        for copy in halos:
            copy.wait_send()
        for copy in chain:
            copy.wait_send()

    for copy in weights:
        copy.wait_send()
    for copy in conv_copies:
        copy.wait_send()
    for u in range(units):
        branch_copy(u, 1, xfs).wait_send()
        branch_copy(u, 2, yfs).wait_send()
        for c in range(ntp):
            forward(c, u).wait_send()
    for g in range(groups):
        norm_copy(g, 1, xfs).wait_send()
        norm_copy(g, 2, yfs).wait_send()
        norm_copy(g, 3, pfs).wait_send()

    @pl.when(jnp.logical_not(home))
    def _():
        conv_home.wait_send()
        for u in range(units):
            branch_copy(u, 0, fs).wait_send()
        for g in range(groups):
            norm_copy(g, 0, fs).wait_send()


def per_device(sizes, *arrays):
    (
        gate,
        head,
        writes,
        reads,
        steps,
        offset,
        rates,
        spikes,
        head_taps,
        write_taps,
        read_taps,
        scale,
        outer,
        inner,
        value,
        conv_taps,
        wstate,
        wconv,
    ) = arrays
    nsp, nfs, ntp = sizes
    length, width = head.shape[1:]
    group_width = writes.shape[2]
    groups = group_width // STATE
    conv_width = inner.shape[2]
    features = wstate.shape[1]
    per_tp = nfs // ntp
    chunks = width // LANES
    half = length // 2
    per_unit = min(2, chunks // groups)
    units = chunks // per_unit
    if (nfs, ntp) != (4, 2):
        raise ValueError('unsupported mesh')
    vm = pl.BlockSpec(memory_space=pltpu.VMEM)
    hbm = pl.BlockSpec(memory_space=pl.ANY)
    dma = pltpu.SemaphoreType.DMA
    return pl.pallas_call(
        functools.partial(kernel, sizes),
        out_shape=jax.ShapeDtypeStruct((per_tp, length, features), BF16),
        in_specs=[hbm] * 4 + [vm] * 8 + [hbm] * 3 + [vm] + [hbm] * 2,
        out_specs=vm,
        scratch_shapes=[
            pltpu.VMEM((1, length, width), BF16),
            pltpu.VMEM((1, length, width), BF16),
            pltpu.VMEM((1, length, group_width), BF16),
            pltpu.VMEM((1, length, group_width), BF16),
            pltpu.VMEM((1, length, conv_width), BF16),
            pltpu.VMEM((1, length, conv_width), BF16),
            pltpu.VMEM((1, length, conv_width), BF16),
            pltpu.VMEM((HALO, width), BF16),
            pltpu.VMEM((HALO, group_width), BF16),
            pltpu.VMEM((HALO, group_width), BF16),
            pltpu.VMEM((HALO, conv_width), BF16),
            pltpu.VMEM((HALO, conv_width), BF16),
            pltpu.VMEM((HALO + length, width), F32),
            pltpu.VMEM((HALO + length, group_width), F32),
            pltpu.VMEM((HALO + length, conv_width), F32),
            pltpu.VMEM((chunks, STATE, LANES), F32),
            pltpu.VMEM((chunks, STATE, LANES), BF16),
            pltpu.VMEM((chunks, STATE, LANES), BF16),
            pltpu.VMEM((units, 2, half, width // units), BF16),
            pltpu.VMEM((per_tp, ntp, units, 2, half, width // units), BF16),
            pltpu.VMEM((groups, 8, length), F32),
            pltpu.VMEM((per_tp, ntp, groups, 8, length), F32),
            pltpu.VMEM((length, conv_width), BF16),
            pltpu.VMEM((per_tp, ntp, length, conv_width), BF16),
            pltpu.VMEM((ntp, width, features), BF16),
            pltpu.VMEM((ntp, conv_width, features), BF16),
            pltpu.VMEM((per_tp, length, features), F32),
            pltpu.VMEM((ntp, length, features), F32),
            pltpu.VMEM((length, width), F32),
            dma((7,)),
            dma((5,)),
            dma((5,)),
            dma((chunks,)),
            dma((chunks,)),
            dma((units, 3)),
            dma((per_tp, ntp, units)),
            dma((ntp, units)),
            dma((2, ntp, units)),
            dma((groups, nfs)),
            dma((per_tp, ntp, groups)),
            dma((nfs,)),
            dma((per_tp, ntp)),
            dma((ntp - 1, 2)),
            dma((ntp - 1, 2)),
            dma((2,)),
        ],
        compiler_params=pltpu.CompilerParams(collective_id=0, has_side_effects=True),
    )(
        gate,
        head,
        writes,
        reads,
        jnp.swapaxes(steps, 1, 2),
        offset[None],
        rates[None],
        spikes.T,
        head_taps,
        write_taps,
        read_taps,
        scale[None],
        outer,
        inner,
        value,
        conv_taps,
        wstate,
        wconv,
    )


def solution(mesh):
    sizes = tuple(mesh.shape[name] for name in ("sp", "fs", "tp"))
    return jax.shard_map(
        functools.partial(per_device, sizes),
        mesh=mesh,
        in_specs=(
            P("fs", "sp", "tp"),
            P("fs", "sp", "tp"),
            P("fs", "sp", "tp"),
            P("fs", "sp", "tp"),
            P("fs", "sp", "tp"),
            P("tp"),
            P("tp"),
            P("sp", "tp"),
            P(None, "tp"),
            P(None, "tp"),
            P(None, "tp"),
            P("tp"),
            P("fs", "sp", "tp"),
            P("fs", "sp", "tp"),
            P("fs", "sp", "tp"),
            P(None, "tp"),
            P("tp", "fs"),
            P("tp", "fs"),
        ),
        out_specs=P("tp", "sp", "fs"),
        check_vma=False,
    )
```

```python
import functools

import jax
import jax.numpy as jnp
from jax import lax
from jax.experimental import pallas as pl
from jax.experimental.pallas import tpu as pltpu
from jax.sharding import PartitionSpec as P

STATE = 128
EPS = 1e-06
LANES = 128
HALO = 8
HIGH = lax.Precision.HIGHEST
MESH = pl.DeviceIdType.MESH
F32 = jnp.float32
BF16 = jnp.bfloat16


def mm(a, b):
    return jnp.dot(a, b, preferred_element_type=F32)


def silu(v):
    return 0.5 * v * (1.0 + jnp.tanh(0.5 * v))


def kernel(
    sizes,
    gate_hbm,
    head_hbm,
    writes_hbm,
    reads_hbm,
    step_ref,
    offset_ref,
    rate_ref,
    spike_ref,
    head_taps,
    write_taps,
    read_taps,
    scale_ref,
    outer_hbm,
    inner_hbm,
    value_hbm,
    conv_taps,
    wstate_hbm,
    wconv_hbm,
    out_ref,
    gate_ref,
    head_ref,
    writes_ref,
    reads_ref,
    outer_ref,
    inner_ref,
    value_ref,
    head_halo,
    write_halo,
    read_halo,
    inner_halo,
    value_halo,
    head_pad,
    write_pad,
    read_pad,
    head_act,
    write_act,
    conv_pad,
    local_state,
    state_send,
    state_recv,
    branch_send,
    branch_recv,
    norm_send,
    norm_recv,
    conv_send,
    conv_recv,
    wstate,
    wconv,
    acc,
    part,
    inside,
    input_sem,
    halo_ss,
    halo_rs,
    state_ss,
    state_rs,
    branch_ss,
    branch_rs,
    half_ss,
    half_rs,
    norm_ss,
    norm_rs,
    conv_ss,
    conv_rs,
    weight_ss,
    weight_rs,
    local_sem,
):
    nsp, nfs, ntp = sizes
    sp, fs, tp = lax.axis_index("sp"), lax.axis_index("fs"), lax.axis_index("tp")
    length, width = head_ref.shape[1:]
    heads = step_ref.shape[1]
    channels = width // heads
    group_width = writes_ref.shape[2]
    groups = group_width // STATE
    ratio = heads // groups
    gw = ratio * channels
    per_tp = nfs // ntp
    chunks = width // LANES
    per_group = chunks // groups
    hpl = LANES // channels
    per_unit = min(2, per_group)
    units = chunks // per_unit
    unit_width = per_unit * LANES
    half = length // 2
    dest = fs // per_tp
    slot = lax.rem(fs, per_tp)
    first, last = sp == 0, sp == nsp - 1

    def at(s, f, t):
        return (s, f, t)

    barrier = pltpu.get_barrier_semaphore()
    for a in range(nfs):
        for b in range(ntp):
            if a == 0 and b == 0:
                continue
            pl.semaphore_signal(
                barrier,
                inc=1,
                device_id=at(sp, lax.rem(fs + a, nfs), lax.rem(tp + b, ntp)),
                device_id_type=MESH,
            )

    @pl.when(jnp.logical_not(first))
    def _():
        pl.semaphore_signal(barrier, inc=1, device_id=at(sp - 1, fs, tp), device_id_type=MESH)

    @pl.when(jnp.logical_not(last))
    def _():
        pl.semaphore_signal(barrier, inc=1, device_id=at(sp + 1, fs, tp), device_id_type=MESH)

    inputs = [
        pltpu.make_async_copy(src, dst, input_sem.at[k])
        for k, (src, dst) in enumerate(
            (
                (writes_hbm, writes_ref),
                (reads_hbm, reads_ref),
                (head_hbm, head_ref),
                (inner_hbm, inner_ref),
                (value_hbm, value_ref),
                (outer_hbm, outer_ref),
                (gate_hbm, gate_ref),
            )
        )
    ]
    for copy in inputs:
        copy.start()

    own_weights = [
        pltpu.make_async_copy(wstate_hbm, wstate.at[tp], local_sem.at[0]),
        pltpu.make_async_copy(wconv_hbm, wconv.at[tp], local_sem.at[1]),
    ]
    for copy in own_weights:
        copy.start()

    ends = jnp.minimum(sp, 1) + jnp.minimum(nsp - 1 - sp, 1)
    for copy in inputs:
        copy.wait()
    pl.semaphore_wait(barrier, nfs * ntp - 1 + ends)

    def remote(src, dst, ss, rs, device):
        return pltpu.make_async_remote_copy(
            src_ref=src, dst_ref=dst, send_sem=ss, recv_sem=rs, device_id=device, device_id_type=MESH
        )

    nxt = at(jnp.minimum(sp + 1, nsp - 1), fs, tp)
    tail = pl.ds(length - HALO, HALO)
    halos = [
        remote(src.at[0, tail, :], dst, halo_ss.at[k], halo_rs.at[k], nxt)
        for k, (src, dst) in enumerate(
            (
                (writes_ref, write_halo),
                (reads_ref, read_halo),
                (head_ref, head_halo),
                (inner_ref, inner_halo),
                (value_ref, value_halo),
            )
        )
    ]

    @pl.when(jnp.logical_not(last))
    def _():
        for copy in halos:
            copy.start()

    def column(ref):
        return jnp.broadcast_to(ref[...], (length, heads)).T

    logits = step_ref[0] + column(offset_ref)
    dt_t = jnp.maximum(logits, 0.0) + jnp.log1p(jnp.exp(-jnp.abs(logits)))
    fall = spike_ref[...] - dt_t * jnp.exp(column(rate_ref))
    rows = lax.broadcasted_iota(jnp.int32, (length, length), 0)
    cols = lax.broadcasted_iota(jnp.int32, (length, length), 1)
    causal = cols <= rows
    rising_t = jnp.dot(
        fall, (rows <= cols).astype(F32), precision=HIGH, preferred_element_type=F32
    )
    rising = rising_t.T
    grow = jnp.exp(rising_t)
    left = dt_t * jnp.exp(rising_t[:, length - 1 : length] - rising_t)
    stacked = jnp.concatenate([grow, left], axis=0)
    coarse = stacked.astype(BF16).astype(F32)
    split = jnp.concatenate([coarse, stacked - coarse], axis=0).T.astype(BF16)
    row_from = lax.broadcasted_iota(jnp.int32, (2 * heads, 2 * width), 0) * channels
    lane = lax.broadcasted_iota(jnp.int32, (2 * heads, 2 * width), 1)
    chosen = jnp.logical_and(lane >= row_from, lane < row_from + channels)
    chosen = jnp.where(chosen, 1.0, 0.0).astype(BF16)
    spread = jnp.concatenate([chosen, chosen], axis=0)
    wide = mm(split, spread)
    grow_wide, left_wide = wide[:, :width], wide[:, width:]
    last_wide = grow_wide[length - 1 : length]

    def taps_over(pad, taps, rows, lanes):
        span = taps.shape[0]
        total = None
        for k in range(span):
            start = HALO - (span - 1) + k
            term = pad[start : start + rows, lanes] * taps[k : k + 1, lanes].astype(F32)
            total = term if total is None else total + term
        return total

    def fill(pad, stream):
        pad[0:HALO, :] = jnp.zeros((HALO, pad.shape[1]), F32)
        pad[HALO : HALO + length, :] = stream

    every = slice(None)
    fill(write_pad, writes_ref[0].astype(F32))
    fill(head_pad, head_ref[0].astype(F32))
    fill(read_pad, reads_ref[0].astype(F32))
    fill(conv_pad, inner_ref[0].astype(F32) * value_ref[0].astype(F32))
    write_act[...] = silu(taps_over(write_pad, write_taps, length, every))
    for g in range(groups):
        span = slice(g * gw, (g + 1) * gw)
        head_act[:, span] = silu(taps_over(head_pad, head_taps, length, span))

    @pl.when(jnp.logical_not(first))
    def _():
        for copy in halos:
            copy.wait_recv()
        for pad, halo in ((write_pad, write_halo), (head_pad, head_halo), (read_pad, read_halo)):
            pad[0:HALO, :] = halo[...].astype(F32)
        conv_pad[0:HALO, :] = inner_halo[...].astype(F32) * value_halo[...].astype(F32)
        write_act[0:HALO, :] = silu(taps_over(write_pad, write_taps, HALO, every))
        head_act[0:HALO, :] = silu(taps_over(head_pad, head_taps, HALO, every))

    hstate = STATE // 2
    chain = [
        [
            remote(state_send.at[i, h], state_recv.at[i, h], state_ss.at[i, h], state_rs.at[i, h], nxt)
            for h in range(2)
        ]
        for i in range(chunks)
    ]
    writes_t = []
    for g in range(groups):
        span = slice(g * gw, (g + 1) * gw)
        writes_t.append(write_act[:, g * STATE : (g + 1) * STATE].T.astype(BF16))
        weighted = (head_act[:, span] * left_wide[:, span]).astype(BF16)
        piece = mm(writes_t[g], weighted)
        for i in range(per_group):
            k = g * per_group + i
            part_of = piece[:, i * LANES : (i + 1) * LANES]
            for h in range(2):
                local_state[k, h] = part_of[h * hstate : (h + 1) * hstate]

        @pl.when(first)
        def _():
            for i in range(g * per_group, (g + 1) * per_group):
                state_send[i] = local_state[i].astype(BF16)
            for i in range(g * per_group, (g + 1) * per_group):
                for copy in chain[i]:
                    copy.start()

    convolved = taps_over(conv_pad, conv_taps, length, every)
    conv_rows = (outer_ref[0].astype(F32) * convolved).astype(BF16)
    conv_send[...] = conv_rows
    conv_copies = []
    for a in range(1, nfs):
        conv_copies.append(
            remote(
                conv_send,
                conv_recv.at[slot, tp],
                conv_ss.at[a],
                conv_rs.at[slot, tp],
                at(sp, lax.rem(fs + a, nfs), dest),
            )
        )
    for copy in conv_copies:
        copy.start()
    conv_home = remote(
        conv_send, conv_recv.at[slot, tp], conv_ss.at[0], conv_rs.at[slot, tp], at(sp, fs, dest)
    )

    @pl.when(dest == tp)
    def _():
        conv_recv[slot, tp] = conv_rows

    @pl.when(dest != tp)
    def _():
        conv_home.start()

    weights = []
    for b in range(1, ntp):
        other = at(sp, fs, lax.rem(tp + b, ntp))
        weights.append(
            remote(wconv_hbm, wconv.at[tp], weight_ss.at[b - 1, 0], weight_rs.at[b - 1, 0], other)
        )
        weights.append(
            remote(wstate_hbm, wstate.at[tp], weight_ss.at[b - 1, 1], weight_rs.at[b - 1, 1], other)
        )
    for copy in weights:
        copy.start()

    reads = silu(taps_over(read_pad, read_taps, length, every)).astype(BF16)
    lane_head = lax.broadcasted_iota(jnp.int32, (length, LANES), 1) // channels
    scores = [
        jnp.where(causal, mm(reads[:, g * STATE : (g + 1) * STATE], writes_t[g]), 0.0)
        for g in range(groups)
    ]

    def within(i):
        block = head_act[:, i * LANES : (i + 1) * LANES].astype(BF16)
        total = None
        for r in range(hpl):
            h = i * hpl + r
            gaps = jnp.minimum(rising[:, h : h + 1] - rising_t[h : h + 1, :], 0.0)
            mixed = (scores[i // per_group] * jnp.exp(gaps) * dt_t[h : h + 1, :]).astype(BF16)
            one = mm(mixed, block)
            total = one if total is None else jnp.where(lane_head == r, one, total)
        inside[:, i * LANES : (i + 1) * LANES] = total

    within(0)

    home = dest == tp
    xfs = fs + 1 - 2 * lax.rem(fs, 2)
    yfs = lax.rem(fs + 2, nfs)
    pfs = nfs - 1 - fs

    def branch_copy(u, k, f):
        return remote(
            branch_send.at[u],
            branch_recv.at[slot, tp, u],
            branch_ss.at[u, k],
            branch_rs.at[slot, tp, u],
            at(sp, f, dest),
        )

    def norm_copy(g, k, f):
        return remote(
            norm_send.at[g],
            norm_recv.at[slot, tp, g],
            norm_ss.at[g, k],
            norm_rs.at[slot, tp, g],
            at(sp, f, dest),
        )

    for g in range(groups):
        span = slice(g * gw, (g + 1) * gw)
        power = jnp.zeros((length, LANES), F32)
        for i in range(g * per_group, (g + 1) * per_group):
            lanes = slice(i * LANES, (i + 1) * LANES)

            @pl.when(jnp.logical_not(first))
            def _():
                for h in range(2):
                    chain[i][h].wait_recv()

                    @pl.when(jnp.logical_not(last))
                    def _():
                        state_send[i, h] = (
                            state_recv[i, h].astype(F32) * last_wide[:, lanes] + local_state[i, h]
                        ).astype(BF16)
                        chain[i][h].start()

                incoming = state_recv[i].reshape(STATE, LANES)
                inside[:, lanes] += (
                    mm(reads[:, g * STATE : (g + 1) * STATE], incoming) * grow_wide[:, lanes]
                )

            gated = inside[:, lanes] * silu(gate_ref[0, :, lanes].astype(F32))
            power = power + gated * gated
            u, at_lane = i // per_unit, (i % per_unit) * LANES
            scaled = (gated * scale_ref[:, lanes]).astype(BF16)
            branch_send[u, 0, :, at_lane : at_lane + LANES] = scaled[:half]
            branch_send[u, 1, :, at_lane : at_lane + LANES] = scaled[half:]
            if i % per_unit == per_unit - 1:
                branch_copy(u, 1, xfs).start()
                branch_copy(u, 2, yfs).start()

                @pl.when(home)
                def _():
                    branch_recv[slot, tp, u] = branch_send[u]

                @pl.when(jnp.logical_not(home))
                def _():
                    branch_copy(u, 0, fs).start()

            if i + 1 < chunks:
                within(i + 1)

        factor = lax.rsqrt(jnp.sum(power, axis=1, keepdims=True) / gw + EPS)
        factor = jnp.broadcast_to(factor, (length, LANES)).T[:8]
        norm_send[g] = factor
        norm_copy(g, 1, xfs).start()
        norm_copy(g, 2, yfs).start()
        norm_copy(g, 3, pfs).start()

        @pl.when(home)
        def _():
            norm_recv[slot, tp, g] = factor

        @pl.when(jnp.logical_not(home))
        def _():
            norm_copy(g, 0, fs).start()

    for copy in own_weights:
        copy.wait()
    for copy in weights:
        copy.wait_recv()

    def local_source(j, c):
        return jnp.logical_and(fs == tp * per_tp + j, tp == c)

    for c in range(ntp):
        for j in range(per_tp):

            @pl.when(jnp.logical_not(local_source(j, c)))
            def _():
                remote(
                    conv_send, conv_recv.at[j, c], conv_ss.at[0], conv_rs.at[j, c], at(sp, fs, dest)
                ).wait_recv()

            term = mm(conv_recv[j, c], wconv[c])
            if c == 0:
                acc[j] = term
            else:
                acc[j] += term
    own = lax.rem(fs, 2)
    side = jnp.where(home, 1 - own, own)
    upper = jnp.where(home, 0, 1)
    onward = at(sp, jnp.where(home, yfs, xfs), tp)

    def forward(c, u):
        return remote(
            branch_recv.at[side, c, u, upper],
            branch_recv.at[side, c, u, upper],
            half_ss.at[c, u],
            half_rs.at[upper, c, u],
            onward,
        )

    def arrived(j, c, u):
        remote(
            branch_send.at[u],
            branch_recv.at[j, c, u],
            branch_ss.at[u, 0],
            branch_rs.at[j, c, u],
            at(sp, xfs, dest),
        ).wait_recv()

    for u in range(units):
        for c in range(ntp):
            arrived(side, c, u)
            forward(c, u).start()

    def project(j, u, c):
        rows = branch_recv[j, c, u].reshape(length, unit_width)
        term = mm(rows, wstate[c, u * unit_width : (u + 1) * unit_width, :])
        if (u * per_unit) % per_group == 0:
            part[c] = term
        else:
            part[c] += term

    def finish(j, g, c):
        @pl.when(jnp.logical_not(local_source(j, c)))
        def _():
            remote(
                norm_send.at[g],
                norm_recv.at[j, c, g],
                norm_ss.at[g, 0],
                norm_rs.at[j, c, g],
                at(sp, xfs, dest),
            ).wait_recv()

        turned = jnp.broadcast_to(norm_recv[j, c, g][:1], (LANES, length)).T
        acc[j] += part[c] * turned[:, :1]

    per_norm = per_group // per_unit
    for j, straight in ((side, True), (1 - side, False)):
        for g in range(groups):
            for u in range(g * per_norm, (g + 1) * per_norm):
                for c in range(ntp):
                    if not straight:

                        @pl.when(jnp.logical_and(home, tp != c))
                        def _():
                            arrived(j, c, u)

                        @pl.when(jnp.logical_not(home))
                        def _():
                            for h in range(2):
                                remote(
                                    branch_send.at[u, h],
                                    branch_recv.at[j, c, u, h],
                                    half_ss.at[c, u],
                                    half_rs.at[h, c, u],
                                    onward,
                                ).wait_recv()

                    project(j, u, c)
            for c in range(ntp):
                finish(j, g, c)
    for j in range(per_tp):
        out_ref[j] = acc[j].astype(BF16)

    @pl.when(jnp.logical_not(last))
    def _():
        for copy in halos:
            copy.wait_send()
        for pair in chain:
            for copy in pair:
                copy.wait_send()

    for copy in weights:
        copy.wait_send()
    for copy in conv_copies:
        copy.wait_send()
    for u in range(units):
        branch_copy(u, 1, xfs).wait_send()
        branch_copy(u, 2, yfs).wait_send()
        for c in range(ntp):
            forward(c, u).wait_send()
    for g in range(groups):
        norm_copy(g, 1, xfs).wait_send()
        norm_copy(g, 2, yfs).wait_send()
        norm_copy(g, 3, pfs).wait_send()

    @pl.when(jnp.logical_not(home))
    def _():
        conv_home.wait_send()
        for u in range(units):
            branch_copy(u, 0, fs).wait_send()
        for g in range(groups):
            norm_copy(g, 0, fs).wait_send()


def per_device(sizes, *arrays):
    (
        gate,
        head,
        writes,
        reads,
        steps,
        offset,
        rates,
        spikes,
        head_taps,
        write_taps,
        read_taps,
        scale,
        outer,
        inner,
        value,
        conv_taps,
        wstate,
        wconv,
    ) = arrays
    nsp, nfs, ntp = sizes
    length, width = head.shape[1:]
    group_width = writes.shape[2]
    groups = group_width // STATE
    conv_width = inner.shape[2]
    features = wstate.shape[1]
    per_tp = nfs // ntp
    chunks = width // LANES
    half = length // 2
    per_unit = min(2, chunks // groups)
    units = chunks // per_unit
    if (nfs, ntp) != (4, 2):
        raise ValueError('unsupported mesh')
    vm = pl.BlockSpec(memory_space=pltpu.VMEM)
    hbm = pl.BlockSpec(memory_space=pl.ANY)
    dma = pltpu.SemaphoreType.DMA
    return pl.pallas_call(
        functools.partial(kernel, sizes),
        out_shape=jax.ShapeDtypeStruct((per_tp, length, features), BF16),
        in_specs=[hbm] * 4 + [vm] * 8 + [hbm] * 3 + [vm] + [hbm] * 2,
        out_specs=vm,
        scratch_shapes=[
            pltpu.VMEM((1, length, width), BF16),
            pltpu.VMEM((1, length, width), BF16),
            pltpu.VMEM((1, length, group_width), BF16),
            pltpu.VMEM((1, length, group_width), BF16),
            pltpu.VMEM((1, length, conv_width), BF16),
            pltpu.VMEM((1, length, conv_width), BF16),
            pltpu.VMEM((1, length, conv_width), BF16),
            pltpu.VMEM((HALO, width), BF16),
            pltpu.VMEM((HALO, group_width), BF16),
            pltpu.VMEM((HALO, group_width), BF16),
            pltpu.VMEM((HALO, conv_width), BF16),
            pltpu.VMEM((HALO, conv_width), BF16),
            pltpu.VMEM((HALO + length, width), F32),
            pltpu.VMEM((HALO + length, group_width), F32),
            pltpu.VMEM((HALO + length, group_width), F32),
            pltpu.VMEM((length, width), F32),
            pltpu.VMEM((length, group_width), F32),
            pltpu.VMEM((HALO + length, conv_width), F32),
            pltpu.VMEM((chunks, 2, STATE // 2, LANES), F32),
            pltpu.VMEM((chunks, 2, STATE // 2, LANES), BF16),
            pltpu.VMEM((chunks, 2, STATE // 2, LANES), BF16),
            pltpu.VMEM((units, 2, half, width // units), BF16),
            pltpu.VMEM((per_tp, ntp, units, 2, half, width // units), BF16),
            pltpu.VMEM((groups, 8, length), F32),
            pltpu.VMEM((per_tp, ntp, groups, 8, length), F32),
            pltpu.VMEM((length, conv_width), BF16),
            pltpu.VMEM((per_tp, ntp, length, conv_width), BF16),
            pltpu.VMEM((ntp, width, features), BF16),
            pltpu.VMEM((ntp, conv_width, features), BF16),
            pltpu.VMEM((per_tp, length, features), F32),
            pltpu.VMEM((ntp, length, features), F32),
            pltpu.VMEM((length, width), F32),
            dma((7,)),
            dma((5,)),
            dma((5,)),
            dma((chunks, 2)),
            dma((chunks, 2)),
            dma((units, 3)),
            dma((per_tp, ntp, units)),
            dma((ntp, units)),
            dma((2, ntp, units)),
            dma((groups, nfs)),
            dma((per_tp, ntp, groups)),
            dma((nfs,)),
            dma((per_tp, ntp)),
            dma((ntp - 1, 2)),
            dma((ntp - 1, 2)),
            dma((2,)),
        ],
        compiler_params=pltpu.CompilerParams(collective_id=0, has_side_effects=True),
    )(
        gate,
        head,
        writes,
        reads,
        jnp.swapaxes(steps, 1, 2),
        offset[None],
        rates[None],
        spikes.T,
        head_taps,
        write_taps,
        read_taps,
        scale[None],
        outer,
        inner,
        value,
        conv_taps,
        wstate,
        wconv,
    )


def solution(mesh):
    sizes = tuple(mesh.shape[name] for name in ("sp", "fs", "tp"))
    return jax.shard_map(
        functools.partial(per_device, sizes),
        mesh=mesh,
        in_specs=(
            P("fs", "sp", "tp"),
            P("fs", "sp", "tp"),
            P("fs", "sp", "tp"),
            P("fs", "sp", "tp"),
            P("fs", "sp", "tp"),
            P("tp"),
            P("tp"),
            P("sp", "tp"),
            P(None, "tp"),
            P(None, "tp"),
            P(None, "tp"),
            P("tp"),
            P("fs", "sp", "tp"),
            P("fs", "sp", "tp"),
            P("fs", "sp", "tp"),
            P(None, "tp"),
            P("tp", "fs"),
            P("tp", "fs"),
        ),
        out_specs=P("tp", "sp", "fs"),
        check_vma=False,
    )
```
